32 devices in a mesh: kv: 8 (over z, y), tp: 4 (over x, core).
Axes of the slice: x: 2, y: 2, z: 4, core: 2. Of those that a mesh axis runs over, the one named last changes fastest.
Arguments:
- hidden_in: bfloat16 [16, 4096], P(None, ('kv', 'tp')), may hold values from -12 to 12
- attn_gain: float32 [4096], P('kv'), may hold values from 0.1 to 1.9
- query_weight: bfloat16 [4096, 4096], P('kv', 'tp'), may hold values from -0.09375 to 0.09375
- key_cache: bfloat16 [16, 8192, 8, 128], P(None, 'kv', 'tp'), may hold values from -600 to 600
- value_cache: bfloat16 [16, 8192, 8, 128], P(None, 'kv', 'tp'), may hold values from -6 to 6
- lambdas: float32 [32], P('tp'), may hold values from 0.3 to 0.8
- head_gain: float32 [128], replicated, may hold values from 0.1 to 1.9
- out_weight: bfloat16 [4096, 4096], P('tp', 'kv'), may hold values from -0.09375 to 0.09375
- mixer_gain: float32 [4096], P(('kv', 'tp')), may hold values from 0.1 to 1.9
- gate_weight: bfloat16 [4096, 11264], P('kv', 'tp'), may hold values from -0.09375 to 0.09375
- up_weight: bfloat16 [4096, 11264], P('kv', 'tp'), may hold values from -0.09375 to 0.09375
- down_weight: bfloat16 [11264, 4096], P('tp', 'kv'), may hold values from -0.0546875 to 0.0546875
Outputs:
- mixed: bfloat16 [16, 4096], P(None, ('kv', 'tp'))
The draws below stay inside these ranges and needn't reach their ends.
All inputs are finite; a program needn't handle non-finite values.
Results may differ from the reference program's by a relative error of at most 0.017.
Values may be sent and summed in bfloat16 or wider, within the bound.
A program may use at most 64 MiB of HBM per device.

```python
import jax
import jax.numpy as jnp
from jax import lax

D = 4096
FF = 11264
HEAD_DIM = 64
KV_HEADS = 8
GROUP = 4
HEADS = 32
BATCH = 16
LENGTH = 8192
COLS_DEV = 128
N_TP = 4


def draw_hidden_in(key, part):
    first = jax.random.fold_in(key, 11)
    second = jax.random.fold_in(key, 12)
    blocks = D // COLS_DEV
    ramp = jnp.arange(blocks, dtype=jnp.float32) / max(blocks - 1, 1)
    jitter = jax.random.uniform(second, (blocks,), jnp.float32, -0.15, 0.15)
    block_scale = jnp.exp(jnp.log(0.5) + ramp * jnp.log(6.0) + jitter)
    base = jax.random.normal(first, (BATCH, D), jnp.float32)
    column_scale = jnp.repeat(block_scale, COLS_DEV)
    values = jnp.clip(base * column_scale[None, :], -12.0, 12.0)
    return values.astype(jnp.bfloat16)


def draw_key_cache(key, part):
    first = jax.random.fold_in(key, 21)
    base = 2.0 * jnp.clip(jax.random.normal(first, (BATCH, LENGTH, KV_HEADS, 2 * HEAD_DIM), jnp.float32), -6.0, 6.0)
    return jnp.clip(base, -600.0, 600.0).astype(jnp.bfloat16)


def level_of(stream_key, shape, pieces, least, top_value):
    level, own = 1.0, jax.random.fold_in(stream_key, 6)
    for axis_at, shards_of in pieces:
        steps = jnp.exp(jax.random.uniform(jax.random.fold_in(own, axis_at), (shards_of,), jnp.float32, least / len(pieces), top_value / len(pieces)))
        level = level * jnp.repeat(steps, shape[axis_at] // shards_of).reshape([-1 if axis == axis_at else 1 for axis in range(len(shape))])
    return level


def centred(rng, shape, scale, reach, pieces=(), held_as=jnp.bfloat16):
    result = scale * jax.random.normal(rng, shape, jnp.float32)
    if pieces:
        result = result * level_of(rng, shape, pieces, -0.22, 0.18)
    return jnp.clip(result, -reach, reach).astype(held_as)


def setup_inputs(seed: int = 0) -> dict:
    arg_keys = jax.random.split(jax.random.key(seed), 13)
    hidden_in = draw_hidden_in(jax.random.fold_in(arg_keys[12], 71), 0)
    attn_gain = jnp.clip(1.0 + 0.18 * jax.random.normal(arg_keys[1], (D,), jnp.float32), 0.1, 1.9)
    query_weight = centred(arg_keys[2], (D, HEADS * 2 * HEAD_DIM), D ** -0.5, 0.09375, ((0, 8), (1, 4)))
    key_cache = draw_key_cache(jax.random.fold_in(arg_keys[12], 71), 0)
    value_cache = centred(arg_keys[4], (BATCH, LENGTH, KV_HEADS, 2 * HEAD_DIM), 1.0, 6.0, ((1, 8), (2, 4)))
    lambdas = jnp.clip(0.3 + 0.5 * jax.random.uniform(arg_keys[5], (HEADS,), jnp.float32) ** level_of(arg_keys[5], (HEADS,), ((0, 4),), -0.2, 0.2), 0.3, 0.8)
    head_gain = jnp.clip(1.0 + 0.18 * jax.random.normal(arg_keys[6], (2 * HEAD_DIM,), jnp.float32), 0.1, 1.9)
    out_weight = centred(arg_keys[7], (HEADS * 2 * HEAD_DIM, D), (HEADS * 2 * HEAD_DIM) ** -0.5, 0.09375, ((0, 4), (1, 8)))
    mixer_gain = jnp.clip(1.0 + 0.18 * jax.random.normal(arg_keys[8], (D,), jnp.float32), 0.1, 1.9)
    gate_weight = centred(arg_keys[9], (D, FF), D ** -0.5, 0.09375, ((0, 8), (1, 4)))
    up_weight = centred(arg_keys[10], (D, FF), D ** -0.5, 0.09375, ((0, 8), (1, 4)))
    down_weight = centred(arg_keys[11], (FF, D), FF ** -0.5, 0.0546875, ((0, 4), (1, 8)))
    return {"hidden_in": hidden_in, "attn_gain": attn_gain, "query_weight": query_weight, "key_cache": key_cache, "value_cache": value_cache, "lambdas": lambdas, "head_gain": head_gain, "out_weight": out_weight, "mixer_gain": mixer_gain, "gate_weight": gate_weight, "up_weight": up_weight, "down_weight": down_weight}


eps = 1e-06

def split_sum(activations, weights):
    block_rows = activations.shape[1] // N_TP
    partials = jnp.einsum('bjr,jrd->jbd', activations.reshape(activations.shape[0], N_TP, block_rows).astype(jnp.float32), weights.reshape(N_TP, block_rows, weights.shape[1]).astype(jnp.float32))
    rounded = lax.optimization_barrier(partials.astype(jnp.bfloat16)).astype(jnp.float32)
    return lax.optimization_barrier(jnp.sum(rounded, axis=0))

def reference(hidden_in, attn_gain, query_weight, key_cache, value_cache, lambdas, head_gain, out_weight, mixer_gain, gate_weight, up_weight, down_weight):
    rows_f = hidden_in.astype(jnp.float32)
    inverse = lax.rsqrt(lax.optimization_barrier(jnp.mean(rows_f * rows_f, axis=1, keepdims=True)) + eps)
    gained = (rows_f * attn_gain).astype(jnp.bfloat16)
    query_full = (jnp.dot(gained, query_weight, preferred_element_type=jnp.float32) * inverse).astype(jnp.bfloat16)
    query_heads = query_full.reshape(BATCH, KV_HEADS, GROUP, 2, HEAD_DIM)
    mixing = lambdas.reshape(KV_HEADS, GROUP)

    def one_group(group_index):
        query_part = lax.dynamic_index_in_dim(query_heads, group_index, 1, keepdims=False).astype(jnp.float32)
        key_part = lax.dynamic_index_in_dim(key_cache, group_index, 2, keepdims=False).astype(jnp.float32)
        key_part = key_part.reshape(BATCH, LENGTH, 2, HEAD_DIM)
        value_part = lax.dynamic_index_in_dim(value_cache, group_index, 2, keepdims=False).astype(jnp.float32)
        scores = jnp.einsum('bgcd,blcd->cbgl', query_part, key_part) * HEAD_DIM ** (-0.5)
        maxima = lax.optimization_barrier(jnp.max(scores, axis=-1, keepdims=True))
        exponent = jnp.exp(scores - maxima)
        totals = lax.optimization_barrier(jnp.sum(exponent, axis=-1))
        rounded = lax.optimization_barrier(exponent.astype(jnp.bfloat16)).astype(jnp.float32)
        weighted = jnp.einsum('cbgl,bld->cbgd', rounded, value_part)
        head_means = weighted / totals[..., None]
        lam_row = lax.dynamic_index_in_dim(mixing, group_index, 0, keepdims=False)
        attended = head_means[0] - lam_row[None, :, None] * head_means[1]
        norm_inv = lax.rsqrt(lax.optimization_barrier(jnp.mean(attended * attended, axis=-1, keepdims=True)) + eps)
        return (attended * norm_inv * head_gain).astype(jnp.bfloat16)
    per_group = lax.map(one_group, jnp.arange(KV_HEADS, dtype=jnp.int32))
    head_out = jnp.moveaxis(per_group, 0, 1).reshape(BATCH, HEADS * 2 * HEAD_DIM)
    attn_out = split_sum(head_out, out_weight)
    after_attn = (rows_f + attn_out).astype(jnp.bfloat16)
    after_f = after_attn.astype(jnp.float32)
    inverse_two = lax.rsqrt(lax.optimization_barrier(jnp.mean(after_f * after_f, axis=1, keepdims=True)) + eps)
    mixer_in = (after_f * inverse_two * mixer_gain).astype(jnp.bfloat16)
    gate_sum = jnp.dot(mixer_in, gate_weight, preferred_element_type=jnp.float32)
    up_sum = jnp.dot(mixer_in, up_weight, preferred_element_type=jnp.float32)
    hidden = (jax.nn.silu(gate_sum) * up_sum).astype(jnp.bfloat16)
    mixer_out = split_sum(hidden, down_weight)
    return (after_f + mixer_out).astype(jnp.bfloat16)
```

```python
import functools
import math

import jax
import jax.numpy as jnp
from jax import lax
from jax.experimental import pallas as pl
from jax.experimental.pallas import tpu as pltpu
from jax.sharding import PartitionSpec as P

MESH = pl.DeviceIdType.MESH
F32, BF16 = jnp.float32, jnp.bfloat16
eps = 1e-06
LANES = 128
CHUNKS = 4
NT = (((1,), (1,)), ((), ()))


def fused_kernel(
    cfg,
    hidden_ref, again_ref, lam_ref, hgain_ref, mgain_ref,
    wq_hbm, k_hbm, v_hbm, wo_hbm, wg_hbm, wu_hbm, wd_hbm,
    out_ref,
    wq, kc, vc, wo, wg, wu, wd,
    xg, gsend, gainb, qs, qr, sqs, sqr, qown, qg, qall,
    acc_s, stat_s, accb, statb, accr, statr,
    hown, hg, ps, pr, aown, ag, sq2s, sq2r, gus, gur, hid_own, hid,
    local_sem, kv_sem, send_kv, recv_kv, send_tp, recv_tp,
):
    n_kv, n_tp, width, head_dim, group, kv_dev = cfg
    batch = hidden_ref.shape[0]
    cols = hidden_ref.shape[1]
    half = batch // 2
    heads = n_kv
    me = lax.axis_index("kv")
    mt = lax.axis_index("tp")
    per = batch // CHUNKS
    slope = head_dim ** -0.5 * math.log2(math.e)

    ff = wg_hbm.shape[1]
    ff_pad = wg.shape[1]
    piece = ff_pad // n_kv

    def local(i, src, dst):
        return pltpu.make_async_copy(src, dst, local_sem.at[i])

    c_wq = local(0, wq_hbm, wq)
    c_wo = local(1, wo_hbm, wo)
    c_wg = local(2, wg_hbm, wg.at[:, pl.ds(0, ff)])
    c_wu = local(3, wu_hbm, wu.at[:, pl.ds(0, ff)])
    c_wd = local(4, wd_hbm, wd.at[pl.ds(0, ff), :])

    def cache_copy(which, hbm, vm, i):
        return pltpu.make_async_copy(
            hbm.at[pl.ds(i * per, per)], vm.at[pl.ds(i * per, per)], kv_sem.at[which, i]
        )

    c_wq.start()
    for i in range(CHUNKS):
        cache_copy(0, k_hbm, kc, i).start()
        cache_copy(1, v_hbm, vc, i).start()
    c_wo.start()
    c_wg.start()
    c_wu.start()
    c_wd.start()

    barrier = pltpu.get_barrier_semaphore()
    for d in range(1, n_kv):
        pl.semaphore_signal(
            barrier, inc=1, device_id={"kv": lax.rem(me + d, n_kv)}, device_id_type=MESH
        )
    for d in range(1, n_tp):
        pl.semaphore_signal(
            barrier, inc=1, device_id={"tp": lax.rem(mt + d, n_tp)}, device_id_type=MESH
        )

    if ff_pad > ff:
        zc = jnp.zeros((wg.shape[0], ff_pad - ff), BF16)
        wg[:, ff:] = zc
        wu[:, ff:] = zc
        wd[ff:, :] = jnp.zeros((ff_pad - ff, wd.shape[1]), BF16)
    gsend[...] = jnp.broadcast_to(mgain_ref[...], gsend.shape)
    pl.semaphore_wait(barrier, n_kv - 1 + n_tp - 1)

    def kv_copy(phase, d, src, dst):
        return pltpu.make_async_remote_copy(
            src_ref=src, dst_ref=dst,
            send_sem=send_kv.at[phase, d], recv_sem=recv_kv.at[phase, d],
            device_id={"kv": lax.rem(me + d, n_kv)}, device_id_type=MESH,
        )

    def tp_copy(phase, d, src, dst):
        return pltpu.make_async_remote_copy(
            src_ref=src, dst_ref=dst,
            send_sem=send_tp.at[phase, d], recv_sem=recv_tp.at[phase, d],
            device_id={"tp": lax.rem(mt + d, n_tp)}, device_id_type=MESH,
        )

    sent = []

    def to_kv(phase, pick_src, pick_dst):
        started = []
        for d in range(1, n_kv):
            peer = lax.rem(me + d, n_kv)
            c = kv_copy(phase, d, pick_src(d, peer), pick_dst(d))
            c.start()
            started.append(c)
        sent.extend(started)
        return started

    def to_tp(phase, pick_src, pick_dst):
        started = []
        for d in range(1, n_tp):
            peer = lax.rem(mt + d, n_tp)
            c = tp_copy(phase, d, pick_src(d, peer), pick_dst(d))
            c.start()
            started.append(c)
        sent.extend(started)
        return started

    def arrive(copies):
        for c in copies:
            c.wait_recv()

    lane8 = lax.broadcasted_iota(jnp.int32, (half, LANES), 1)

    def pack_rows(sq):
        return jnp.where(
            lane8 < LANES // 2,
            jnp.broadcast_to(sq[:half], (half, LANES)),
            jnp.broadcast_to(sq[half:], (half, LANES)),
        )

    def unpack_rows(s):
        return jnp.concatenate([s[:, 0:1], s[:, LANES // 2 : LANES // 2 + 1]], axis=0)

    cx = to_tp(0, lambda d, p: hidden_ref, lambda d: xg.at[mt])
    cgain = to_tp(1, lambda d, p: gsend, lambda d: gainb.at[mt])
    xg[mt] = hidden_ref[...]
    gainb[mt] = gsend[...]
    arrive(cx)
    xf = jnp.concatenate([xg[t] for t in range(n_tp)], axis=1).astype(F32)
    gained = (xf * again_ref[...]).astype(BF16)
    sqs[...] = pack_rows(jnp.sum(xf * xf, axis=1, keepdims=True))
    csq = to_kv(0, lambda d, p: sqs, lambda d: sqr.at[d])

    c_wq.wait()
    qp = jnp.dot(gained, wq[...], preferred_element_type=F32)
    hw = 2 * head_dim
    for j in range(heads):
        qs[j] = qp[:, j * hw : (j + 1) * hw]
    cq = to_kv(1, lambda d, p: qs.at[p], lambda d: qr.at[d])
    arrive(csq)
    sq = sqs[...]
    for d in range(1, n_kv):
        sq = sq + sqr[d]
    scale1 = lax.rsqrt(unpack_rows(sq) / width + eps)
    q = qs[me]
    for d, c in enumerate(cq, 1):
        c.wait_recv()
        q = q + qr[d]
    qown[...] = (q * scale1).astype(BF16)
    cqg = to_kv(2, lambda d, p: qown, lambda d: qg.at[me])
    qg[me] = qown[...]
    lane16 = lax.broadcasted_iota(jnp.int32, (batch, hw), 1)
    arrive(cqg)
    for j in range(heads):
        qj = qg[j].astype(F32)
        for c in range(2):
            r = 2 * j + c
            keep = (lane16 // head_dim) == c
            qall[r * batch : (r + 1) * batch, :] = jnp.where(keep, qj, 0.0)

    rows = 2 * heads
    flat = kc.shape[1]
    row_i = lax.broadcasted_iota(jnp.int32, (rows, flat), 0)
    lane_i = lax.broadcasted_iota(jnp.int32, (rows, flat), 1)
    own_key = lax.rem(lane_i, kv_dev) == row_i // (2 * group)
    lane_r = lax.broadcasted_iota(jnp.int32, (rows, LANES), 1)
    is_max = lax.rem(lane_r, LANES // 2) < LANES // 4

    def attend(i, carry):
        cache_copy(0, k_hbm, kc, i).wait()
        cache_copy(1, v_hbm, vc, i).wait()
        for u in range(per):
            b = i * per + u
            qb = qall[pl.ds(b, rows, stride=batch), :].astype(BF16)
            s = lax.dot_general(qb, kc[b], NT, preferred_element_type=F32)
            s = jnp.where(own_key, s, -jnp.inf)
            m = jnp.max(s, axis=1, keepdims=True)
            p = jnp.exp2((s - m) * slope)
            t = jnp.sum(p, axis=1, keepdims=True)
            a = jnp.dot(p.astype(BF16), vc[b], preferred_element_type=F32)
            acc_s[pl.ds(b, rows, stride=batch), :] = a
            stat_s[pl.ds(b, rows, stride=batch), :] = jnp.where(
                is_max, jnp.broadcast_to(m, (rows, LANES)), jnp.broadcast_to(t, (rows, LANES))
            )
        return carry

    lax.fori_loop(0, CHUNKS, attend, 0)

    lane_b = lax.broadcasted_iota(jnp.int32, (batch, LANES), 1)
    for j in range(heads):
        lo = 2 * j * batch
        accb[j] = acc_s[lo : lo + 2 * batch, :].astype(BF16)
        statb[j] = jnp.where(
            lane_b < LANES // 2, stat_s[lo : lo + batch, :], stat_s[lo + batch : lo + 2 * batch, :]
        )
    cst = to_kv(3, lambda d, p: statb.at[p], lambda d: statr.at[d])
    cac = to_kv(4, lambda d, p: accb.at[p], lambda d: accr.at[d])
    statr[0] = statb[me]
    accr[0] = accb[me]
    arrive(cst)
    quarter = LANES // 4
    means = []
    factors = []
    totals = []
    for c in range(2):
        base = c * (LANES // 2)
        ms = [statr[d][:, base : base + 1] for d in range(n_kv)]
        ts = [statr[d][:, base + quarter : base + quarter + 1] for d in range(n_kv)]
        top = functools.reduce(jnp.maximum, ms)
        fs = [jnp.exp2((m - top) * slope) for m in ms]
        totals.append(functools.reduce(jnp.add, [t * f for t, f in zip(ts, fs)]))
        factors.append(fs)
    arrive(cac)
    for c in range(2):
        num = functools.reduce(
            jnp.add,
            [accr[d][c * batch : (c + 1) * batch].astype(F32) * factors[c][d] for d in range(n_kv)],
        )
        means.append(num / totals[c])
    attended = means[0] - lam_ref[me] * means[1]
    norm_inv = lax.rsqrt(jnp.mean(attended * attended, axis=-1, keepdims=True) + eps)
    hown[...] = (attended * norm_inv * hgain_ref[...]).astype(BF16)

    chg = to_kv(5, lambda d, p: hown, lambda d: hg.at[me])
    hg[me] = hown[...]
    c_wo.wait()
    arrive(chg)
    ho = jnp.concatenate([hg[j] for j in range(heads)], axis=1)
    proj = jnp.dot(ho, wo[...], preferred_element_type=F32).astype(BF16)
    for t in range(n_tp):
        ps[0, t] = proj[:, t * cols : (t + 1) * cols]
    cp = to_tp(2, lambda d, p: ps.at[0, p], lambda d: pr.at[0, d])
    attn = ps[0, mt].astype(F32)
    for d, c in enumerate(cp, 1):
        c.wait_recv()
        attn = attn + pr[0, d].astype(F32)
    aown[...] = (hidden_ref[...].astype(F32) + attn).astype(BF16)

    ca = to_tp(3, lambda d, p: aown, lambda d: ag.at[mt])
    ag[mt] = aown[...]
    arrive(cgain)
    gain = jnp.concatenate([gainb[t][0:1] for t in range(n_tp)], axis=1)
    arrive(ca)
    af = jnp.concatenate([ag[t] for t in range(n_tp)], axis=1).astype(F32)
    mixin = (af * gain).astype(BF16)
    sq2s[...] = pack_rows(jnp.sum(af * af, axis=1, keepdims=True))
    csq2 = to_kv(6, lambda d, p: sq2s, lambda d: sq2r.at[d])
    c_wg.wait()
    c_wu.wait()
    cgu = []
    for d in list(range(1, n_kv)) + [0]:
        peer = lax.rem(me + d, n_kv)
        at = pl.ds(pl.multiple_of(peer * piece, LANES), piece)
        gp = jnp.dot(mixin, wg[:, at], preferred_element_type=F32)
        up = jnp.dot(mixin, wu[:, at], preferred_element_type=F32)
        if d == 0:
            gate_sum, up_sum = gp, up
        else:
            gus[d, 0] = gp.astype(BF16)
            gus[d, 1] = up.astype(BF16)
            c = kv_copy(7, d, gus.at[d], gur.at[d])
            c.start()
            cgu.append(c)
    sent.extend(cgu)
    arrive(csq2)
    sq = sq2s[...]
    for d in range(1, n_kv):
        sq = sq + sq2r[d]
    scale2 = lax.rsqrt(unpack_rows(sq) / width + eps)
    for d, c in enumerate(cgu, 1):
        c.wait_recv()
        gate_sum = gate_sum + gur[d, 0].astype(F32)
        up_sum = up_sum + gur[d, 1].astype(F32)
    gate_sum = gate_sum * scale2
    up_sum = up_sum * scale2
    hid_own[...] = (gate_sum / (1.0 + jnp.exp(-gate_sum)) * up_sum).astype(BF16)
    chid = to_kv(8, lambda d, p: hid_own, lambda d: hid.at[me])
    c_wd.wait()
    at0 = pl.ds(pl.multiple_of(me * piece, LANES), piece)
    down = jnp.dot(hid_own[...], wd[at0, :], preferred_element_type=F32)
    for d, c in enumerate(chid, 1):
        c.wait_recv()
        src = lax.rem(me + n_kv - d, n_kv)
        at = pl.ds(pl.multiple_of(src * piece, LANES), piece)
        down = down + jnp.dot(hid[src], wd[at, :], preferred_element_type=F32)
    downb = down.astype(BF16)
    for t in range(n_tp):
        ps[1, t] = downb[:, t * cols : (t + 1) * cols]
    cd = to_tp(4, lambda d, p: ps.at[1, p], lambda d: pr.at[1, d])
    mix = ps[1, mt].astype(F32)
    for d, c in enumerate(cd, 1):
        c.wait_recv()
        mix = mix + pr[1, d].astype(F32)
    out_ref[...] = (aown[...].astype(F32) + mix).astype(BF16)
    for c in sent:
        c.wait_send()


def fused(n_kv, n_tp, hidden_in, attn_gain, query_weight, key_cache, value_cache, lambdas,
          head_gain, out_weight, mixer_gain, gate_weight, up_weight, down_weight):
    batch, cols = hidden_in.shape
    positions, kv_dev, hw = key_cache.shape[1:]
    heads = lambdas.shape[0]
    group = heads // kv_dev
    width = cols * n_kv * n_tp
    block, ff = gate_weight.shape
    piece = -(-ff // (LANES * n_kv)) * LANES
    ff_pad = piece * n_kv
    keys = key_cache.reshape(batch, positions * kv_dev, hw)
    values = value_cache.reshape(batch, positions * kv_dev, hw)
    half = batch // 2
    V = pltpu.VMEM
    scratch = [
        V(query_weight.shape, BF16), V(keys.shape, BF16), V(values.shape, BF16),
        V(out_weight.shape, BF16), V((block, ff_pad), BF16), V((block, ff_pad), BF16),
        V((ff_pad, down_weight.shape[1]), BF16),
        V((n_tp, batch, cols), BF16), V((8, cols), F32), V((n_tp, 8, cols), F32),
        V((heads, batch, hw), F32), V((n_kv, batch, hw), F32),
        V((half, LANES), F32), V((n_kv, half, LANES), F32),
        V((batch, hw), BF16), V((heads, batch, hw), BF16), V((2 * heads * batch, hw), F32),
        V((2 * heads * batch, hw), F32), V((2 * heads * batch, LANES), F32),
        V((heads, 2 * batch, hw), BF16), V((heads, batch, LANES), F32),
        V((n_kv, 2 * batch, hw), BF16), V((n_kv, batch, LANES), F32),
        V((batch, hw), BF16), V((heads, batch, hw), BF16),
        V((2, n_tp, batch, cols), BF16), V((2, n_tp, batch, cols), BF16),
        V((batch, cols), BF16), V((n_tp, batch, cols), BF16),
        V((half, LANES), F32), V((n_kv, half, LANES), F32),
        V((n_kv, 2, batch, piece), BF16), V((n_kv, 2, batch, piece), BF16),
        V((batch, piece), BF16), V((n_kv, batch, piece), BF16),
        pltpu.SemaphoreType.DMA((5,)), pltpu.SemaphoreType.DMA((2, CHUNKS)),
        pltpu.SemaphoreType.DMA((9, n_kv)), pltpu.SemaphoreType.DMA((9, n_kv)),
        pltpu.SemaphoreType.DMA((5, n_tp)), pltpu.SemaphoreType.DMA((5, n_tp)),
    ]
    vmem = pl.BlockSpec(memory_space=pltpu.VMEM)
    smem = pl.BlockSpec(memory_space=pltpu.SMEM)
    hbm = pl.BlockSpec(memory_space=pl.ANY)
    cfg = (n_kv, n_tp, width, hw // 2, group, kv_dev)
    return pl.pallas_call(
        functools.partial(fused_kernel, cfg),
        out_shape=jax.ShapeDtypeStruct((batch, cols), BF16),
        in_specs=[vmem, vmem, smem, vmem, vmem] + [hbm] * 7,
        out_specs=vmem,
        scratch_shapes=scratch,
        compiler_params=pltpu.CompilerParams(
            collective_id=0, has_side_effects=True, vmem_limit_bytes=60 * 1024 * 1024
        ),
    )(
        hidden_in, attn_gain.reshape(1, block), lambdas, head_gain.reshape(1, hw),
        mixer_gain.reshape(1, cols), query_weight, keys, values, out_weight,
        gate_weight, up_weight, down_weight,
    )

HEAD_DIM = 64


def finish_heads(totals, weighted, lambdas, head_gain, kv_dev, group_size):
    head_means = weighted / totals[..., None]
    mixing = lambdas.reshape(kv_dev, group_size)
    attended = head_means[0] - mixing[None, :, :, None] * head_means[1]
    norm_inv = lax.rsqrt(jnp.mean(attended * attended, axis=-1, keepdims=True) + eps)
    head_out = (attended * norm_inv * head_gain).astype(jnp.bfloat16)
    return head_out.reshape(head_out.shape[0], kv_dev * group_size * 2 * HEAD_DIM)


def per_device(
    hidden_in,
    attn_gain,
    query_weight,
    key_cache,
    value_cache,
    lambdas,
    head_gain,
    out_weight,
    mixer_gain,
    gate_weight,
    up_weight,
    down_weight,
):
    batch_rows = hidden_in.shape[0]
    width = hidden_in.shape[1] * lax.axis_size(("kv", "tp"))
    rows_block = lax.all_gather(hidden_in, "tp", axis=1, tiled=True)
    block_f = rows_block.astype(jnp.float32)
    gained = (block_f * attn_gain).astype(jnp.bfloat16)
    partial_value = jnp.dot(gained, query_weight, preferred_element_type=jnp.float32)
    own_cols = hidden_in.astype(jnp.float32)
    squares = lax.psum(jnp.sum(own_cols * own_cols, axis=1), ("kv", "tp"))
    query_full = lax.psum(partial_value, "kv")
    row_scale = lax.rsqrt(squares / width + eps)
    query_rows = (query_full * row_scale[:, None]).astype(jnp.bfloat16)
    positions = key_cache.shape[1]
    kv_dev = key_cache.shape[2]
    heads_dev = query_rows.shape[1] // (2 * HEAD_DIM)
    group_size = heads_dev // kv_dev
    query_heads = query_rows.reshape(batch_rows, kv_dev, group_size, 2, HEAD_DIM)
    key_rows = key_cache.reshape(batch_rows, positions, kv_dev, 2, HEAD_DIM)
    scores = jnp.einsum(
        "bkgcd,bpkcd->cbkgp", query_heads, key_rows, preferred_element_type=jnp.float32
    ) * HEAD_DIM ** (-0.5)
    maxima = jnp.max(scores, axis=-1)
    exponent = jnp.exp(scores - maxima[..., None])
    totals = jnp.sum(exponent, axis=-1)
    exp_weights = exponent.astype(jnp.bfloat16)
    weighted = jnp.einsum(
        "cbkgp,bpkv->cbkgv", exp_weights, value_cache, preferred_element_type=jnp.float32
    )
    parts_max, parts_tot, parts_acc = (
        lax.all_to_all(maxima[None], "kv", split_axis=2, concat_axis=0, tiled=True),
        lax.all_to_all(totals[None], "kv", split_axis=2, concat_axis=0, tiled=True),
        lax.all_to_all(weighted[None], "kv", split_axis=2, concat_axis=0, tiled=True),
    )
    top = jnp.max(parts_max, axis=0)
    factors = jnp.exp(parts_max - top[None])
    own_tot = jnp.sum(parts_tot * factors, axis=0)
    own_acc = jnp.sum(parts_acc * factors[..., None], axis=0)
    own_out = finish_heads(own_tot, own_acc, lambdas, head_gain, kv_dev, group_size)
    head_out = lax.all_gather(own_out, "kv", axis=0, tiled=True)
    projected = jnp.dot(head_out, out_weight, preferred_element_type=jnp.float32)
    attn_out = lax.psum_scatter(
        projected.astype(jnp.bfloat16), "tp", scatter_dimension=1, tiled=True
    ).astype(jnp.float32)
    after_attn = (hidden_in.astype(jnp.float32) + attn_out).astype(jnp.bfloat16)
    after_f = after_attn.astype(jnp.float32)
    squares_two = lax.psum(jnp.sum(after_f * after_f, axis=1), ("kv", "tp"))
    mixer_in = (after_f * lax.rsqrt(squares_two / width + eps)[:, None] * mixer_gain).astype(
        jnp.bfloat16
    )
    gathered = lax.all_gather(mixer_in, "tp", axis=1, tiled=True)
    gate_part = jnp.dot(gathered, gate_weight, preferred_element_type=jnp.float32)
    up_part = jnp.dot(gathered, up_weight, preferred_element_type=jnp.float32)
    gate_sum, up_sum = lax.psum((gate_part, up_part), "kv")
    hidden = (jax.nn.silu(gate_sum) * up_sum).astype(jnp.bfloat16)
    down_part = jnp.dot(hidden, down_weight, preferred_element_type=jnp.float32)
    mixer_out = lax.psum_scatter(
        down_part.astype(jnp.bfloat16), "tp", scatter_dimension=1, tiled=True
    ).astype(jnp.float32)
    return (after_f + mixer_out).astype(jnp.bfloat16)


def solution(mesh):
    n_kv, n_tp = mesh.shape["kv"], mesh.shape["tp"]

    def layer(*arrays):
        heads_dev = arrays[5].shape[0]
        if heads_dev == n_kv:
            return fused(n_kv, n_tp, *arrays)
        return per_device(*arrays)

    in_specs = (
        P(None, ("kv", "tp")),
        P("kv"),
        P("kv", "tp"),
        P(None, "kv", "tp", None),
        P(None, "kv", "tp", None),
        P("tp"),
        P(),
        P("tp", "kv"),
        P(("kv", "tp")),
        P("kv", "tp"),
        P("kv", "tp"),
        P("tp", "kv"),
    )
    out_specs = P(None, ("kv", "tp"))
    return jax.shard_map(
        layer, mesh=mesh, in_specs=in_specs, out_specs=out_specs, check_vma=False
    )
```

```python
import functools
import math

import jax
import jax.numpy as jnp
from jax import lax
from jax.experimental import pallas as pl
from jax.experimental.pallas import tpu as pltpu
from jax.sharding import PartitionSpec as P

MESH = pl.DeviceIdType.MESH
F32, BF16 = jnp.float32, jnp.bfloat16
eps = 1e-06
LANES = 128
CHUNKS = 4
NT = (((1,), (1,)), ((), ()))


def fused_kernel(
    cfg,
    hidden_ref, again_ref, lam_ref, hgain_ref, mgain_ref,
    wq_hbm, k_hbm, v_hbm, wo_hbm, wg_hbm, wu_hbm, wd_hbm,
    out_ref,
    wq, kc, vc, wo, wg, wu, wd,
    xg, gsend, gainb, qs, qr, sqs, sqr, qown, qg, qall,
    acc_s, stat_s, accb, statb, accr, statr,
    hown, hg, projs, projr, ps, pr, ag, sq2s, sq2r, gus, gur, hid_own, hid,
    local_sem, kv_sem, send_kv, recv_kv, send_tp, recv_tp,
):
    n_kv, n_tp, width, head_dim, group, kv_dev = cfg
    batch = hidden_ref.shape[0]
    cols = hidden_ref.shape[1]
    half = batch // 2
    heads = n_kv
    me = lax.axis_index("kv")
    mt = lax.axis_index("tp")
    per = batch // CHUNKS
    slope = head_dim ** -0.5 * math.log2(math.e)

    ff = wg_hbm.shape[1]
    ff_pad = wg.shape[1]
    piece = ff_pad // n_kv

    def local(i, src, dst):
        return pltpu.make_async_copy(src, dst, local_sem.at[i])

    c_wq = local(0, wq_hbm, wq)
    c_wo = local(1, wo_hbm, wo)
    c_wg = local(2, wg_hbm, wg.at[:, pl.ds(0, ff)])
    c_wu = local(3, wu_hbm, wu.at[:, pl.ds(0, ff)])
    c_wd = local(4, wd_hbm, wd.at[pl.ds(0, ff), :])

    def cache_copy(which, hbm, vm, i):
        return pltpu.make_async_copy(
            hbm.at[pl.ds(i * per, per)], vm.at[pl.ds(i * per, per)], kv_sem.at[which, i]
        )

    c_wq.start()
    for i in range(CHUNKS):
        cache_copy(0, k_hbm, kc, i).start()
        cache_copy(1, v_hbm, vc, i).start()
    c_wo.start()
    c_wg.start()
    c_wu.start()
    c_wd.start()

    barrier = pltpu.get_barrier_semaphore()
    for d in range(1, n_kv):
        pl.semaphore_signal(
            barrier, inc=1, device_id={"kv": lax.rem(me + d, n_kv)}, device_id_type=MESH
        )
    for d in range(1, n_tp):
        pl.semaphore_signal(
            barrier, inc=1, device_id={"tp": lax.rem(mt + d, n_tp)}, device_id_type=MESH
        )

    if ff_pad > ff:
        zc = jnp.zeros((wg.shape[0], ff_pad - ff), BF16)
        wg[:, ff:] = zc
        wu[:, ff:] = zc
        wd[ff:, :] = jnp.zeros((ff_pad - ff, wd.shape[1]), BF16)
    gsend[...] = jnp.broadcast_to(mgain_ref[...], gsend.shape)
    pl.semaphore_wait(barrier, n_kv - 1 + n_tp - 1)

    def kv_copy(phase, d, src, dst):
        return pltpu.make_async_remote_copy(
            src_ref=src, dst_ref=dst,
            send_sem=send_kv.at[phase, d], recv_sem=recv_kv.at[phase, d],
            device_id={"kv": lax.rem(me + d, n_kv)}, device_id_type=MESH,
        )

    def tp_copy(phase, d, src, dst):
        return pltpu.make_async_remote_copy(
            src_ref=src, dst_ref=dst,
            send_sem=send_tp.at[phase, d], recv_sem=recv_tp.at[phase, d],
            device_id={"tp": lax.rem(mt + d, n_tp)}, device_id_type=MESH,
        )

    sent = []
    order = sorted(range(1, n_kv), key=lambda d: (abs(2 * d - n_kv), d))

    def to_kv(phase, pick_src, pick_dst):
        started = {}
        for d in order:
            peer = lax.rem(me + d, n_kv)
            c = kv_copy(phase, d, pick_src(d, peer), pick_dst(d))
            c.start()
            started[d] = c
        sent.extend(started.values())
        return [started[d] for d in range(1, n_kv)]

    def to_tp(phase, pick_src, pick_dst):
        started = []
        for d in range(1, n_tp):
            peer = lax.rem(mt + d, n_tp)
            c = tp_copy(phase, d, pick_src(d, peer), pick_dst(d))
            c.start()
            started.append(c)
        sent.extend(started)
        return started

    def arrive(copies):
        for c in copies:
            c.wait_recv()

    lane8 = lax.broadcasted_iota(jnp.int32, (half, LANES), 1)

    def pack_rows(sq):
        return jnp.where(
            lane8 < LANES // 2,
            jnp.broadcast_to(sq[:half], (half, LANES)),
            jnp.broadcast_to(sq[half:], (half, LANES)),
        )

    def unpack_rows(s):
        return jnp.concatenate([s[:, 0:1], s[:, LANES // 2 : LANES // 2 + 1]], axis=0)

    cx = to_tp(0, lambda d, p: hidden_ref, lambda d: xg.at[mt])
    cgain = to_tp(1, lambda d, p: gsend, lambda d: gainb.at[mt])
    xg[mt] = hidden_ref[...]
    gainb[mt] = gsend[...]
    arrive(cx)
    xf = jnp.concatenate([xg[t] for t in range(n_tp)], axis=1).astype(F32)
    gained = (xf * again_ref[...]).astype(BF16)
    sqs[...] = pack_rows(jnp.sum(xf * xf, axis=1, keepdims=True))
    csq = to_kv(0, lambda d, p: sqs, lambda d: sqr.at[d])

    c_wq.wait()
    qp = jnp.dot(gained, wq[...], preferred_element_type=F32)
    hw = 2 * head_dim
    for j in range(heads):
        qs[j] = qp[:, j * hw : (j + 1) * hw]
    cq = to_kv(1, lambda d, p: qs.at[p], lambda d: qr.at[d])
    arrive(csq)
    sq = sqs[...]
    for d in range(1, n_kv):
        sq = sq + sqr[d]
    scale1 = lax.rsqrt(unpack_rows(sq) / width + eps)
    q = qs[me]
    for d, c in enumerate(cq, 1):
        c.wait_recv()
        q = q + qr[d]
    qown[...] = (q * scale1).astype(BF16)
    cqg = to_kv(2, lambda d, p: qown, lambda d: qg.at[me])
    qg[me] = qown[...]
    lane16 = lax.broadcasted_iota(jnp.int32, (batch, hw), 1)
    arrive(cqg)
    for j in range(heads):
        qj = qg[j].astype(F32)
        for c in range(2):
            r = 2 * j + c
            keep = (lane16 // head_dim) == c
            qall[r * batch : (r + 1) * batch, :] = jnp.where(keep, qj, 0.0)

    rows = 2 * heads
    flat = kc.shape[1]
    row_i = lax.broadcasted_iota(jnp.int32, (rows, flat), 0)
    lane_i = lax.broadcasted_iota(jnp.int32, (rows, flat), 1)
    own_key = lax.rem(lane_i, kv_dev) == row_i // (2 * group)
    lane_r = lax.broadcasted_iota(jnp.int32, (rows, LANES), 1)
    is_max = lax.rem(lane_r, LANES // 2) < LANES // 4

    def attend(i, carry):
        cache_copy(0, k_hbm, kc, i).wait()
        cache_copy(1, v_hbm, vc, i).wait()
        for u in range(per):
            b = i * per + u
            qb = qall[pl.ds(b, rows, stride=batch), :].astype(BF16)
            s = lax.dot_general(qb, kc[b], NT, preferred_element_type=F32)
            s = jnp.where(own_key, s, -jnp.inf)
            m = jnp.max(s, axis=1, keepdims=True)
            p = jnp.exp2((s - m) * slope)
            t = jnp.sum(p, axis=1, keepdims=True)
            a = jnp.dot(p.astype(BF16), vc[b], preferred_element_type=F32)
            acc_s[pl.ds(b, rows, stride=batch), :] = a
            stat_s[pl.ds(b, rows, stride=batch), :] = jnp.where(
                is_max, jnp.broadcast_to(m, (rows, LANES)), jnp.broadcast_to(t, (rows, LANES))
            )
        return carry

    lax.fori_loop(0, CHUNKS, attend, 0)

    lane_b = lax.broadcasted_iota(jnp.int32, (batch, LANES), 1)
    for j in range(heads):
        lo = 2 * j * batch
        accb[j] = acc_s[lo : lo + 2 * batch, :].astype(BF16)
        statb[j] = jnp.where(
            lane_b < LANES // 2, stat_s[lo : lo + batch, :], stat_s[lo + batch : lo + 2 * batch, :]
        )
    cst = to_kv(3, lambda d, p: statb.at[p], lambda d: statr.at[d])
    cac = to_kv(4, lambda d, p: accb.at[p], lambda d: accr.at[d])
    statr[0] = statb[me]
    accr[0] = accb[me]
    arrive(cst)
    quarter = LANES // 4
    means = []
    factors = []
    totals = []
    for c in range(2):
        base = c * (LANES // 2)
        ms = [statr[d][:, base : base + 1] for d in range(n_kv)]
        ts = [statr[d][:, base + quarter : base + quarter + 1] for d in range(n_kv)]
        top = functools.reduce(jnp.maximum, ms)
        fs = [jnp.exp2((m - top) * slope) for m in ms]
        totals.append(functools.reduce(jnp.add, [t * f for t, f in zip(ts, fs)]))
        factors.append(fs)
    arrive(cac)
    for c in range(2):
        num = functools.reduce(
            jnp.add,
            [accr[d][c * batch : (c + 1) * batch].astype(F32) * factors[c][d] for d in range(n_kv)],
        )
        means.append(num / totals[c])
    attended = means[0] - lam_ref[me] * means[1]
    norm_inv = lax.rsqrt(jnp.mean(attended * attended, axis=-1, keepdims=True) + eps)
    hown[...] = (attended * norm_inv * hgain_ref[...]).astype(BF16)

    chg = to_kv(5, lambda d, p: hown, lambda d: hg.at[me])
    hg[me] = hown[...]
    c_wo.wait()
    arrive(chg)
    ho = jnp.concatenate([hg[j] for j in range(heads)], axis=1)
    projs[...] = jnp.dot(ho, wo[...], preferred_element_type=F32).astype(BF16)
    cp = to_tp(2, lambda d, p: projs, lambda d: projr.at[mt])
    projr[mt] = projs[...]
    arrive(cgain)
    gain = jnp.concatenate([gainb[t][0:1] for t in range(n_tp)], axis=1)
    arrive(cp)

    attn = projr[0].astype(F32)
    for t in range(1, n_tp):
        attn = attn + projr[t].astype(F32)
    after = (xf + attn).astype(BF16)
    for t in range(n_tp):
        ag[t] = after[:, t * cols : (t + 1) * cols]
    af = after.astype(F32)
    mixin = (af * gain).astype(BF16)
    sq2s[...] = pack_rows(jnp.sum(af * af, axis=1, keepdims=True))
    csq2 = to_kv(6, lambda d, p: sq2s, lambda d: sq2r.at[d])
    c_wg.wait()
    c_wu.wait()
    cgu = {}
    for d in order + [0]:
        peer = lax.rem(me + d, n_kv)
        at = pl.ds(pl.multiple_of(peer * piece, LANES), piece)
        gp = jnp.dot(mixin, wg[:, at], preferred_element_type=F32)
        up = jnp.dot(mixin, wu[:, at], preferred_element_type=F32)
        if d == 0:
            gate_sum, up_sum = gp, up
        else:
            gus[d, 0] = gp.astype(BF16)
            gus[d, 1] = up.astype(BF16)
            c = kv_copy(7, d, gus.at[d], gur.at[d])
            c.start()
            cgu[d] = c
    sent.extend(cgu.values())
    arrive(csq2)
    sq = sq2s[...]
    for d in range(1, n_kv):
        sq = sq + sq2r[d]
    scale2 = lax.rsqrt(unpack_rows(sq) / width + eps)
    for d, c in sorted(cgu.items()):
        c.wait_recv()
        gate_sum = gate_sum + gur[d, 0].astype(F32)
        up_sum = up_sum + gur[d, 1].astype(F32)
    gate_sum = gate_sum * scale2
    up_sum = up_sum * scale2
    hid_own[...] = (gate_sum / (1.0 + jnp.exp(-gate_sum)) * up_sum).astype(BF16)
    chid = to_kv(8, lambda d, p: hid_own, lambda d: hid.at[me])
    c_wd.wait()
    at0 = pl.ds(pl.multiple_of(me * piece, LANES), piece)
    down = jnp.dot(hid_own[...], wd[at0, :], preferred_element_type=F32)
    for d, c in enumerate(chid, 1):
        c.wait_recv()
        src = lax.rem(me + n_kv - d, n_kv)
        at = pl.ds(pl.multiple_of(src * piece, LANES), piece)
        down = down + jnp.dot(hid[src], wd[at, :], preferred_element_type=F32)
    downb = down.astype(BF16)
    for t in range(n_tp):
        ps[t] = downb[:, t * cols : (t + 1) * cols]
    cd = to_tp(3, lambda d, p: ps.at[p], lambda d: pr.at[d])
    mix = ps[mt].astype(F32)
    for d, c in enumerate(cd, 1):
        c.wait_recv()
        mix = mix + pr[d].astype(F32)
    out_ref[...] = (ag[mt].astype(F32) + mix).astype(BF16)
    for c in sent:
        c.wait_send()


def fused(n_kv, n_tp, hidden_in, attn_gain, query_weight, key_cache, value_cache, lambdas,
          head_gain, out_weight, mixer_gain, gate_weight, up_weight, down_weight):
    batch, cols = hidden_in.shape
    positions, kv_dev, hw = key_cache.shape[1:]
    heads = lambdas.shape[0]
    group = heads // kv_dev
    width = cols * n_kv * n_tp
    block, ff = gate_weight.shape
    piece = -(-ff // (LANES * n_kv)) * LANES
    ff_pad = piece * n_kv
    keys = key_cache.reshape(batch, positions * kv_dev, hw)
    values = value_cache.reshape(batch, positions * kv_dev, hw)
    half = batch // 2
    V = pltpu.VMEM
    scratch = [
        V(query_weight.shape, BF16), V(keys.shape, BF16), V(values.shape, BF16),
        V(out_weight.shape, BF16), V((block, ff_pad), BF16), V((block, ff_pad), BF16),
        V((ff_pad, down_weight.shape[1]), BF16),
        V((n_tp, batch, cols), BF16), V((8, cols), F32), V((n_tp, 8, cols), F32),
        V((heads, batch, hw), F32), V((n_kv, batch, hw), F32),
        V((half, LANES), F32), V((n_kv, half, LANES), F32),
        V((batch, hw), BF16), V((heads, batch, hw), BF16), V((2 * heads * batch, hw), F32),
        V((2 * heads * batch, hw), F32), V((2 * heads * batch, LANES), F32),
        V((heads, 2 * batch, hw), BF16), V((heads, batch, LANES), F32),
        V((n_kv, 2 * batch, hw), BF16), V((n_kv, batch, LANES), F32),
        V((batch, hw), BF16), V((heads, batch, hw), BF16),
        V((batch, block), BF16), V((n_tp, batch, block), BF16),
        V((n_tp, batch, cols), BF16), V((n_tp, batch, cols), BF16),
        V((n_tp, batch, cols), BF16),
        V((half, LANES), F32), V((n_kv, half, LANES), F32),
        V((n_kv, 2, batch, piece), BF16), V((n_kv, 2, batch, piece), BF16),
        V((batch, piece), BF16), V((n_kv, batch, piece), BF16),
        pltpu.SemaphoreType.DMA((5,)), pltpu.SemaphoreType.DMA((2, CHUNKS)),
        pltpu.SemaphoreType.DMA((9, n_kv)), pltpu.SemaphoreType.DMA((9, n_kv)),
        pltpu.SemaphoreType.DMA((4, n_tp)), pltpu.SemaphoreType.DMA((4, n_tp)),
    ]
    vmem = pl.BlockSpec(memory_space=pltpu.VMEM)
    smem = pl.BlockSpec(memory_space=pltpu.SMEM)
    hbm = pl.BlockSpec(memory_space=pl.ANY)
    cfg = (n_kv, n_tp, width, hw // 2, group, kv_dev)
    return pl.pallas_call(
        functools.partial(fused_kernel, cfg),
        out_shape=jax.ShapeDtypeStruct((batch, cols), BF16),
        in_specs=[vmem, vmem, smem, vmem, vmem] + [hbm] * 7,
        out_specs=vmem,
        scratch_shapes=scratch,
        compiler_params=pltpu.CompilerParams(
            collective_id=0, has_side_effects=True, vmem_limit_bytes=60 * 1024 * 1024
        ),
    )(
        hidden_in, attn_gain.reshape(1, block), lambdas, head_gain.reshape(1, hw),
        mixer_gain.reshape(1, cols), query_weight, keys, values, out_weight,
        gate_weight, up_weight, down_weight,
    )

HEAD_DIM = 64


def finish_heads(totals, weighted, lambdas, head_gain, kv_dev, group_size):
    head_means = weighted / totals[..., None]
    mixing = lambdas.reshape(kv_dev, group_size)
    attended = head_means[0] - mixing[None, :, :, None] * head_means[1]
    norm_inv = lax.rsqrt(jnp.mean(attended * attended, axis=-1, keepdims=True) + eps)
    head_out = (attended * norm_inv * head_gain).astype(jnp.bfloat16)
    return head_out.reshape(head_out.shape[0], kv_dev * group_size * 2 * HEAD_DIM)


def per_device(
    hidden_in,
    attn_gain,
    query_weight,
    key_cache,
    value_cache,
    lambdas,
    head_gain,
    out_weight,
    mixer_gain,
    gate_weight,
    up_weight,
    down_weight,
):
    batch_rows = hidden_in.shape[0]
    width = hidden_in.shape[1] * lax.axis_size(("kv", "tp"))
    rows_block = lax.all_gather(hidden_in, "tp", axis=1, tiled=True)
    block_f = rows_block.astype(jnp.float32)
    gained = (block_f * attn_gain).astype(jnp.bfloat16)
    partial_value = jnp.dot(gained, query_weight, preferred_element_type=jnp.float32)
    own_cols = hidden_in.astype(jnp.float32)
    squares = lax.psum(jnp.sum(own_cols * own_cols, axis=1), ("kv", "tp"))
    query_full = lax.psum(partial_value, "kv")
    row_scale = lax.rsqrt(squares / width + eps)
    query_rows = (query_full * row_scale[:, None]).astype(jnp.bfloat16)
    positions = key_cache.shape[1]
    kv_dev = key_cache.shape[2]
    heads_dev = query_rows.shape[1] // (2 * HEAD_DIM)
    group_size = heads_dev // kv_dev
    query_heads = query_rows.reshape(batch_rows, kv_dev, group_size, 2, HEAD_DIM)
    key_rows = key_cache.reshape(batch_rows, positions, kv_dev, 2, HEAD_DIM)
    scores = jnp.einsum(
        "bkgcd,bpkcd->cbkgp", query_heads, key_rows, preferred_element_type=jnp.float32
    ) * HEAD_DIM ** (-0.5)
    maxima = jnp.max(scores, axis=-1)
    exponent = jnp.exp(scores - maxima[..., None])
    totals = jnp.sum(exponent, axis=-1)
    exp_weights = exponent.astype(jnp.bfloat16)
    weighted = jnp.einsum(
        "cbkgp,bpkv->cbkgv", exp_weights, value_cache, preferred_element_type=jnp.float32
    )
    parts_max, parts_tot, parts_acc = (
        lax.all_to_all(maxima[None], "kv", split_axis=2, concat_axis=0, tiled=True),
        lax.all_to_all(totals[None], "kv", split_axis=2, concat_axis=0, tiled=True),
        lax.all_to_all(weighted[None], "kv", split_axis=2, concat_axis=0, tiled=True),
    )
    top = jnp.max(parts_max, axis=0)
    factors = jnp.exp(parts_max - top[None])
    own_tot = jnp.sum(parts_tot * factors, axis=0)
    own_acc = jnp.sum(parts_acc * factors[..., None], axis=0)
    own_out = finish_heads(own_tot, own_acc, lambdas, head_gain, kv_dev, group_size)
    head_out = lax.all_gather(own_out, "kv", axis=0, tiled=True)
    projected = jnp.dot(head_out, out_weight, preferred_element_type=jnp.float32)
    attn_out = lax.psum_scatter(
        projected.astype(jnp.bfloat16), "tp", scatter_dimension=1, tiled=True
    ).astype(jnp.float32)
    after_attn = (hidden_in.astype(jnp.float32) + attn_out).astype(jnp.bfloat16)
    after_f = after_attn.astype(jnp.float32)
    squares_two = lax.psum(jnp.sum(after_f * after_f, axis=1), ("kv", "tp"))
    mixer_in = (after_f * lax.rsqrt(squares_two / width + eps)[:, None] * mixer_gain).astype(
        jnp.bfloat16
    )
    gathered = lax.all_gather(mixer_in, "tp", axis=1, tiled=True)
    gate_part = jnp.dot(gathered, gate_weight, preferred_element_type=jnp.float32)
    up_part = jnp.dot(gathered, up_weight, preferred_element_type=jnp.float32)
    gate_sum, up_sum = lax.psum((gate_part, up_part), "kv")
    hidden = (jax.nn.silu(gate_sum) * up_sum).astype(jnp.bfloat16)
    down_part = jnp.dot(hidden, down_weight, preferred_element_type=jnp.float32)
    mixer_out = lax.psum_scatter(
        down_part.astype(jnp.bfloat16), "tp", scatter_dimension=1, tiled=True
    ).astype(jnp.float32)
    return (after_f + mixer_out).astype(jnp.bfloat16)


def solution(mesh):
    n_kv, n_tp = mesh.shape["kv"], mesh.shape["tp"]

    def layer(*arrays):
        heads_dev = arrays[5].shape[0]
        if heads_dev == n_kv:
            return fused(n_kv, n_tp, *arrays)
        return per_device(*arrays)

    in_specs = (
        P(None, ("kv", "tp")),
        P("kv"),
        P("kv", "tp"),
        P(None, "kv", "tp", None),
        P(None, "kv", "tp", None),
        P("tp"),
        P(),
        P("tp", "kv"),
        P(("kv", "tp")),
        P("kv", "tp"),
        P("kv", "tp"),
        P("tp", "kv"),
    )
    out_specs = P(None, ("kv", "tp"))
    return jax.shard_map(
        layer, mesh=mesh, in_specs=in_specs, out_specs=out_specs, check_vma=False
    )
```
